32 devices in a mesh: sp: 8 (over z, x), tp: 4 (over y, core).
Axes of the slice: x: 2, y: 2, z: 4, core: 2. Of those that a mesh axis runs over, the one named last changes fastest.
Arguments:
- conv_value: bfloat16 [4096, 1024], P('sp', 'tp'), may hold values from -6 to 6
- conv_gate: bfloat16 [4096, 1024], P('sp', 'tp'), may hold values from -9 to 9
- conv_weight: float32 [31, 1024], P(None, 'tp'), may hold values from -2.2 to 2.2
- conv_gain: float32 [1024], P('tp'), may hold values from 0.1 to 1.9
- conv_shift: float32 [1024], P('tp'), may hold values from -3 to 3
- out_weight: bfloat16 [1024, 2048], P('tp'), may hold values from -0.1875 to 0.1875
- residual: bfloat16 [4096, 2048], P('sp', 'tp'), may hold values from -10 to 10
- mix_gain: float32 [2048], P('tp'), may hold values from 0.1 to 1.9
- expert_ids: int32 [4096, 2], P('sp'), may hold values from 0 to 7, all different within a row; in each aligned block of 128 rows (0 to 127, 128 to 255, ...) at most 64 rows name the same one
- group_weight: float32 [4096], P('sp'), may hold values from 0.6 to 1
- score_gap: float32 [4096], P('sp'), may hold values from -0.8 to 0.8
- w_gate: bfloat16 [8, 2048, 1024], P('sp', None, 'tp'), may hold values from -0.125 to 0.125
- w_up: bfloat16 [8, 2048, 1024], P('sp', None, 'tp'), may hold values from -0.125 to 0.125
- w_down: bfloat16 [8, 1024, 2048], P('sp', 'tp'), may hold values from -0.1875 to 0.1875
Outputs:
- layer_out: bfloat16 [4096, 2048], P('sp', 'tp')
The draws below stay inside these ranges and needn't reach their ends.
Inputs may be any that keep to these rules, and one draw needn't show every extreme that they name: `expert_ids`: the two experts of a position differ. In each aligned block of 512 // 4 positions no expert is named by more than 64 rows, a bound that some block reaches.
All inputs are finite; a program needn't handle non-finite values.
Results may differ from the reference program's by a relative error of at most 0.012.
Values may be sent and summed in bfloat16 or wider, within the bound.
No kernel may reach another device: no remote copies, remote signals or barrier semaphores. Data moves between devices by JAX's collectives and lax.ppermute only.
A program may use at most 128 MiB of HBM per device.

```python
import math
import jax
import jax.numpy as jnp
import numpy as np
from jax import lax

D = 2048
CH = 1024
FF = 1024
KW = 31
ROWS = 512
TOKENS = 4096
EXPERTS = 8
CAP = 64
N_SP = 8
N_TP = 4


def draw_conv_weight(key, part):
    rising = jnp.exp(jnp.linspace(math.log(0.3), math.log(3.0), CH)).astype(jnp.float32)
    base = jnp.clip(jax.random.normal(key, (KW, CH), jnp.float32), -4.0, 4.0)
    return (base * rising[None, :] / math.sqrt(KW)).astype(jnp.float32)


def draw_residual(key, part):
    rising = jnp.exp(jnp.linspace(math.log(0.5), math.log(2.0), D)).astype(jnp.float32)
    base = jnp.clip(jax.random.normal(key, (TOKENS, D), jnp.float32), -5.0, 5.0)
    return (base * rising[None, :]).astype(jnp.bfloat16)


def levels(key, extent, shards, smallest, high):
    def one(axis_at, blocks):
        steps = jax.random.uniform(jax.random.fold_in(jax.random.fold_in(key, 6), axis_at), (blocks,), jnp.float32, smallest / len(shards), high / len(shards))
        return jnp.repeat(jnp.exp(steps), extent[axis_at] // blocks).reshape((-1,) + (1,) * (len(extent) - axis_at - 1))

    level = one(*shards[0])
    for cut in shards[1:]:
        level = level * one(*cut)
    return level


def assign_block(stream_key, own, number, rows, amount, top, bound, lean):
    sequence = jax.random.permutation(stream_key, amount)
    heavy_load, common = load_shares(amount, rows * top, bound, lean, True), load_shares(amount, rows * top, bound, lean, False)
    places = jnp.arange(amount)

    def named(tallies, offset_by):
        used = int((tallies > 0).sum())
        fixed = max(1, used // 4)
        passed = fixed + (places - fixed + offset_by * (used - fixed)) % max(1, amount - fixed)
        return jnp.zeros((amount,), jnp.int32).at[sequence[jnp.where(places < fixed, places, passed)]].set(jnp.asarray(tallies, jnp.int32))

    tallies = jnp.where(number % 4 == 0, named(heavy_load, number // 4), named(common, number - number // 4 - 1))
    mixed = jax.random.permutation(jax.random.fold_in(own, 3), amount)
    donor, receiver = mixed[0:amount // 2 * 2:2], mixed[1:amount // 2 * 2:2]
    margin = jnp.minimum(tallies[donor] - 1, bound - tallies[receiver]) // 2
    margin = jnp.where((donor == sequence[0]) | (receiver == sequence[0]) | (tallies[receiver] == 0), 0, jnp.maximum(margin, 0))
    passed = jax.random.randint(jax.random.fold_in(own, 4), (amount // 2,), 0, 1 << 20) % (margin + 1)
    tallies = tallies.at[donor].add(-passed).at[receiver].add(passed)
    items = jnp.searchsorted(jnp.cumsum(tallies), jnp.arange(rows * top), side="right").astype(jnp.int32)
    grid = items.reshape(top, rows).T
    grid = grid[jax.random.permutation(jax.random.fold_in(own, 1), rows)]
    offset_by = jax.random.randint(jax.random.fold_in(own, 2), (rows, 1), 0, top)
    return jnp.take_along_axis(grid, (jnp.arange(top)[None, :] + offset_by) % top, axis=1)


def load_shares(count, total, most, skew, full):
    loads = [(1 << 20) // math.isqrt(standing ** skew) + 1 for standing in range(1, count + 1)]
    largest = most if full else min(most, max(-(-total // count), total * loads[0] // sum(loads)))
    least = 1 if total - largest >= count - 1 else 0
    holding, surplus = [largest] + [least] * (count - 1), total - largest - least * (count - 1)
    while surplus > 0:
        candidates = [i for i in range(1, count) if holding[i] < largest] or [i for i in range(1, count) if holding[i] < most]
        pool, left = sum([loads[i] for i in candidates]), surplus
        for i in candidates:
            extra = min(most - holding[i], max(1, left * loads[i] // pool), surplus)
            holding[i] = holding[i] + extra
            surplus = surplus - extra
    return np.array(holding)


def scatter_about(own_key, shape, spread, reach, split=(), kind=jnp.bfloat16):
    entries = jax.random.normal(own_key, shape, jnp.float32) * spread
    if len(split) > 0:
        entries = levels(own_key, shape, split, -0.22, 0.18) * entries
    return jnp.clip(entries, min=-reach, max=reach).astype(kind)


def setup_inputs(seed: int = 0) -> dict:
    splits = jax.random.split(jax.random.key(seed), 15)
    conv_value = scatter_about(splits[0], (TOKENS, CH), 1.0, 6.0, ((0, 8), (1, 4)))
    conv_gate = scatter_about(splits[1], (TOKENS, CH), 1.5, 9.0, ((0, 8), (1, 4)))
    conv_weight = draw_conv_weight(jax.random.fold_in(splits[14], 71), 0)
    conv_gain = jnp.clip(1.0 + 0.18 * jax.random.normal(splits[3], (CH,), jnp.float32), 0.1, 1.9)
    conv_shift = scatter_about(splits[4], (CH,), 0.5, 3.0, ((0, 4),), jnp.float32)
    out_weight = scatter_about(splits[5], (CH, D), CH ** -0.5, 0.1875, ((0, 4),))
    residual = draw_residual(jax.random.fold_in(splits[14], 71), 0)
    mix_gain = jnp.clip(1.0 + 0.18 * jax.random.normal(splits[7], (D,), jnp.float32), 0.1, 1.9)
    expert_ids_keys = jax.random.split(jax.random.fold_in(splits[8], 1), TOKENS // (ROWS // N_TP))
    expert_ids_turns = jax.random.permutation(jax.random.fold_in(splits[8], 3), TOKENS // (ROWS // N_TP))
    expert_ids = jax.vmap(lambda own, number: assign_block(jax.random.fold_in(splits[8], 2), own, number, ROWS // N_TP, EXPERTS, 2, CAP, 2))(expert_ids_keys, expert_ids_turns).reshape((TOKENS, 2))
    group_weight = jnp.clip(0.6 + 0.39999998 * jax.random.uniform(splits[9], (TOKENS,), jnp.float32) ** levels(splits[9], (TOKENS,), ((0, 8),), -0.2, 0.2), 0.6, 1.0)
    score_gap = jnp.clip(jax.random.uniform(splits[10], (TOKENS,), jnp.float32, -0.8, 0.8) * levels(splits[10], (TOKENS,), ((0, 8),), -0.4, 0.0), -0.8, 0.8)
    w_gate = scatter_about(splits[11], (EXPERTS, D, FF), D ** -0.5, 0.125, ((0, 8), (2, 4)))
    w_up = scatter_about(splits[12], (EXPERTS, D, FF), D ** -0.5, 0.125, ((0, 8), (2, 4)))
    w_down = scatter_about(splits[13], (EXPERTS, FF, D), FF ** -0.5, 0.1875, ((0, 8), (1, 4)))
    return {"conv_value": conv_value, "conv_gate": conv_gate, "conv_weight": conv_weight, "conv_gain": conv_gain, "conv_shift": conv_shift, "out_weight": out_weight, "residual": residual, "mix_gain": mix_gain, "expert_ids": expert_ids, "group_weight": group_weight, "score_gap": score_gap, "w_gate": w_gate, "w_up": w_up, "w_down": w_down}


eps = 1e-06

def reference(conv_value, conv_gate, conv_weight, conv_gain, conv_shift, out_weight, residual, mix_gain, expert_ids, group_weight, score_gap, w_gate, w_up, w_down):
    gated = conv_value.astype(jnp.float32) * jax.nn.sigmoid(conv_gate.astype(jnp.float32))
    padded = jnp.pad(gated, ((KW - 1, 0), (0, 0)))
    convolved = jnp.zeros_like(gated)
    for tap_index in range(KW):
        convolved = convolved + conv_weight[tap_index] * padded[tap_index:tap_index + TOKENS]
    row_mean = lax.optimization_barrier(jnp.mean(convolved, axis=-1, keepdims=True))
    row_var = lax.optimization_barrier(jnp.mean(convolved * convolved, axis=-1, keepdims=True)) - row_mean * row_mean
    normalized = (convolved - row_mean) * lax.rsqrt(row_var + eps) * conv_gain + conv_shift
    activated = jax.nn.silu(normalized).astype(jnp.bfloat16)
    block_width = CH // N_TP
    mixed = jnp.zeros((TOKENS, D), jnp.float32)
    for block_index in range(N_TP):
        low = block_index * block_width
        term = jnp.dot(activated[:, low:low + block_width], out_weight[low:low + block_width], preferred_element_type=jnp.float32)
        mixed = mixed + term.astype(jnp.bfloat16).astype(jnp.float32)
    middle = (residual.astype(jnp.float32) + mixed).astype(jnp.bfloat16)
    middle_wide = middle.astype(jnp.float32)
    normed = (middle_wide * lax.rsqrt(lax.optimization_barrier(jnp.mean(middle_wide * middle_wide, axis=-1, keepdims=True)) + eps) * mix_gain).astype(jnp.bfloat16)
    assign_count = TOKENS * 2
    expert_cap = N_SP * N_TP * CAP
    flat_experts = expert_ids.reshape(-1)
    token_of = jnp.concatenate([jnp.arange(assign_count, dtype=jnp.int32) // 2, jnp.array([TOKENS], jnp.int32)])
    normed_pad = jnp.concatenate([normed, jnp.zeros((1, D), jnp.bfloat16)], axis=0).astype(jnp.float32)
    hidden_width = FF // N_TP

    def expert_step(carry, expert):
        positions = jnp.nonzero(flat_experts == expert, size=expert_cap, fill_value=assign_count)[0].astype(jnp.int32)
        chosen = normed_pad[token_of[positions]]
        gate_part = jnp.dot(chosen, w_gate[expert].astype(jnp.float32))
        up_part = jnp.dot(chosen, w_up[expert].astype(jnp.float32))
        hidden = (jax.nn.silu(gate_part) * up_part).astype(jnp.bfloat16).astype(jnp.float32)
        down = w_down[expert].astype(jnp.float32)
        total = jnp.zeros((expert_cap, D), jnp.float32)
        for block_index in range(N_TP):
            low = block_index * hidden_width
            term = jnp.dot(hidden[:, low:low + hidden_width], down[low:low + hidden_width])
            total = total + term.astype(jnp.bfloat16).astype(jnp.float32)
        carry = carry.at[positions].set(total.astype(jnp.bfloat16))
        return (carry, None)
    start = jnp.zeros((assign_count + 1, D), jnp.bfloat16)
    results, _ = lax.scan(expert_step, start, jnp.arange(EXPERTS, dtype=jnp.int32))
    picked = results[:assign_count].reshape(TOKENS, 2, D).astype(jnp.float32)
    first_gate = group_weight * jax.nn.sigmoid(score_gap)
    second_gate = group_weight * jax.nn.sigmoid(-score_gap)
    layer_out = middle_wide + first_gate[:, None] * picked[:, 0] + second_gate[:, None] * picked[:, 1]
    return layer_out.astype(jnp.bfloat16)
```

```python
import jax
import jax.numpy as jnp
from jax import lax
from jax.sharding import PartitionSpec as P


D = 2048
CH = 1024


eps = 1e-06


def swap(value, bit):
    count = lax.axis_size("tp")
    return lax.ppermute(value, "tp", [(source, source ^ bit) for source in range(count)])


def natural(blocks, index):
    ordered = []
    for place in range(len(blocks)):
        chosen = blocks[0]
        for bit in range(1, len(blocks)):
            chosen = jnp.where(index == (place ^ bit), blocks[bit], chosen)
        ordered.append(chosen)
    return ordered


def exchanged(piece):
    count = lax.axis_size("tp")
    blocks = [piece(0)]
    for bit in range(1, count):
        blocks.append(swap(piece(bit), bit))
    return blocks


def gathered(block):
    count = lax.axis_size("tp")
    held = {0: block}
    bit = count // 2
    while bit:
        for have in sorted(held):
            held[bit ^ have] = swap(held[have], bit)
        bit //= 2
    return [held[bit] for bit in range(count)]


def dot(left, right):
    return jnp.dot(left, right, preferred_element_type=jnp.float32)


def shards(
    conv_value,
    conv_gate,
    conv_weight,
    conv_gain,
    conv_shift,
    out_weight,
    residual,
    mix_gain,
    expert_ids,
    group_weight,
    score_gap,
    w_gate,
    w_up,
    w_down,
):
    row_count, width = conv_value.shape
    taps = conv_weight.shape[0]
    reach = taps - 1
    halo = -(-reach // 16) * 16
    seq_devices = lax.axis_size("sp")
    tp_devices = lax.axis_size("tp")
    quarter = row_count // tp_devices
    capacity = 4 * quarter // seq_devices
    slots = seq_devices * capacity
    col_count = residual.shape[1]
    tp = lax.axis_index("tp")

    gated = conv_value.astype(jnp.float32) * jax.nn.sigmoid(conv_gate.astype(jnp.float32))
    gated = gated.astype(jnp.bfloat16)
    previous = lax.ppermute(
        gated[row_count - halo :], "sp", [(i, i + 1) for i in range(seq_devices - 1)]
    )
    padded = jnp.concatenate([previous, gated], axis=0)
    windows = exchanged(
        lambda bit: lax.dynamic_slice_in_dim(padded, (tp ^ bit) * quarter, halo + quarter, 0),
    )
    small = jnp.concatenate(
        [conv_weight, conv_gain[None], conv_shift[None], mix_gain.reshape(-1, width)], axis=0
    )
    smalls = exchanged(lambda bit: small)

    out_weights = gathered(out_weight)
    residuals = natural(
        exchanged(lambda bit: lax.dynamic_slice_in_dim(residual, (tp ^ bit) * quarter, quarter, 0)),
        tp,
    )
    gates = gathered(w_gate[0])
    ups = gathered(w_up[0])
    downs = gathered(w_down[0])

    ids = lax.dynamic_slice_in_dim(expert_ids, tp * quarter, quarter, 0)
    experts = jnp.arange(seq_devices, dtype=jnp.int32)[None]
    first_hot = (ids[:, :1] == experts).astype(jnp.bfloat16)
    second_hot = (ids[:, 1:] == experts).astype(jnp.bfloat16)
    earlier = jnp.tri(quarter, k=-1, dtype=jnp.bfloat16)
    before = dot(earlier, first_hot + second_hot)
    slot_ids = jnp.arange(slots, dtype=jnp.int32)[None]
    first_rank = jnp.sum(before * first_hot, axis=1).astype(jnp.int32)
    second_rank = jnp.sum(before * second_hot, axis=1).astype(jnp.int32)
    first_pick = ((ids[:, 0] * capacity + first_rank)[:, None] == slot_ids).astype(jnp.bfloat16)
    second_pick = ((ids[:, 1] * capacity + second_rank)[:, None] == slot_ids).astype(jnp.bfloat16)
    weights = lax.dynamic_slice_in_dim(group_weight, tp * quarter, quarter, 0)
    gaps = lax.dynamic_slice_in_dim(score_gap, tp * quarter, quarter, 0)
    first_gate = (weights * jax.nn.sigmoid(gaps))[:, None]
    second_gate = (weights * jax.nn.sigmoid(-gaps))[:, None]

    convolved = []
    for window, part in zip(windows, smalls):
        wide = window.astype(jnp.float32)
        total = jnp.zeros((quarter, width), jnp.float32)
        for tap in range(taps):
            start = halo - reach + tap
            total = total + part[tap] * wide[start : start + quarter]
        convolved.append(total)
    row_mean = sum(jnp.sum(c, axis=-1, keepdims=True) for c in convolved) / CH
    row_var = sum(jnp.sum(c * c, axis=-1, keepdims=True) for c in convolved) / CH
    row_var = row_var - row_mean * row_mean
    scale = lax.rsqrt(row_var + eps)
    mixed = 0.0
    for c, part, weight in zip(convolved, smalls, out_weights):
        normalized = (c - row_mean) * scale * part[taps] + part[taps + 1]
        mixed = mixed + dot(jax.nn.silu(normalized).astype(jnp.bfloat16), weight)
    middle = (jnp.concatenate(residuals, axis=1).astype(jnp.float32) + mixed).astype(jnp.bfloat16)
    middle_wide = middle.astype(jnp.float32)
    row_sq = jnp.sum(middle_wide * middle_wide, axis=-1, keepdims=True)
    gain = jnp.concatenate([g[taps + 2 :].reshape(-1) for g in natural(smalls, tp)])
    normed = (middle_wide * lax.rsqrt(row_sq / D + eps) * gain).astype(jnp.bfloat16)

    outgoing = lax.dot_general(
        first_pick + second_pick,
        normed,
        (((0,), (0,)), ((), ())),
        preferred_element_type=jnp.float32,
    ).astype(jnp.bfloat16)
    received = lax.all_to_all(
        outgoing.reshape(seq_devices, capacity, D), "sp", 0, 0, tiled=True
    ).reshape(slots, D)
    total = 0.0
    for gate, up, down in zip(gates, ups, downs):
        hidden = (jax.nn.silu(dot(received, gate)) * dot(received, up)).astype(jnp.bfloat16)
        total = total + dot(hidden, down)
    returned = lax.all_to_all(
        total.astype(jnp.bfloat16).reshape(seq_devices, capacity, D), "sp", 0, 0, tiled=True
    ).reshape(slots, D)

    picked = first_gate * dot(first_pick, returned) + second_gate * dot(second_pick, returned)
    result = (middle_wide + picked).astype(jnp.bfloat16)
    rows = natural(
        exchanged(
            lambda bit: lax.dynamic_slice_in_dim(result, (tp ^ bit) * col_count, col_count, 1),
        ),
        tp,
    )
    return jnp.concatenate(rows, axis=0)


def solution(mesh):
    return jax.shard_map(
        shards,
        mesh=mesh,
        in_specs=(
            P("sp", "tp"),
            P("sp", "tp"),
            P(None, "tp"),
            P("tp"),
            P("tp"),
            P("tp", None),
            P("sp", "tp"),
            P("tp"),
            P("sp", None),
            P("sp"),
            P("sp"),
            P("sp", None, "tp"),
            P("sp", None, "tp"),
            P("sp", "tp", None),
        ),
        out_specs=P("sp", "tp"),
        check_vma=False,
    )
```

```python
import jax
import jax.numpy as jnp
from jax import lax
from jax.experimental import pallas as pl
from jax.experimental.pallas import tpu as pltpu
from jax.sharding import Mesh
from jax.sharding import PartitionSpec as P


D = 2048
CH = 1024


eps = 1e-06
FEW = 8


def swap(value, bit):
    count = lax.axis_size("tp")
    return lax.ppermute(value, "tp", [(source, source ^ bit) for source in range(count)])


def natural(blocks, index):
    ordered = []
    for place in range(len(blocks)):
        chosen = blocks[0]
        for bit in range(1, len(blocks)):
            chosen = jnp.where(index == (place ^ bit), blocks[bit], chosen)
        ordered.append(chosen)
    return ordered


def exchanged(piece):
    count = lax.axis_size("tp")
    blocks = [piece(0)]
    for bit in range(1, count):
        blocks.append(swap(piece(bit), bit))
    return blocks


def gathered(block):
    count = lax.axis_size("tp")
    held = {0: block}
    bit = count // 2
    while bit:
        for have in sorted(held):
            held[bit ^ have] = swap(held[have], bit)
        bit //= 2
    return [held[bit] for bit in range(count)]


def dot(left, right):
    return jnp.dot(left, right, preferred_element_type=jnp.float32)


def hidden_kernel(places, blocks, *refs):
    pieces = max(len(places), 1)
    x_refs, refs = refs[:pieces], refs[pieces:]
    weight_refs, refs = refs[: 2 * blocks], refs[2 * blocks :]
    own_ref, other_ref, refs = refs[0], refs[1], refs[2:]
    x, (held, sems) = (refs[0], refs[1:]) if places else (x_refs[0], refs)
    width = weight_refs[0].shape[1]
    copies = [
        pltpu.make_async_copy(ref, held.at[i // 2, :, pl.ds(i % 2 * width, width)], sems.at[i])
        for i, ref in enumerate(weight_refs)
    ]
    for copy in copies:
        copy.start()
    for (top, left), x_ref in zip(places, x_refs):
        height, columns = x_ref.shape
        x[top : top + height, left : left + columns] = x_ref[...]
    half = own_ref.shape[0]
    for block in range(blocks):
        copies[2 * block].wait()
        copies[2 * block + 1].wait()
        for i, out_ref in enumerate((own_ref, other_ref)):
            both = dot(x[i * half : (i + 1) * half], held[block])
            gate, up = both[:, :width], both[:, width:]
            out_ref[:, block * width : (block + 1) * width] = (jax.nn.silu(gate) * up).astype(
                jnp.bfloat16
            )


def whole(shape):
    return pl.BlockSpec(shape, lambda i: (0,) * len(shape))


def hidden_rows(pieces, places, rows, gates, ups):
    depth, width = gates[0].shape
    blocks = len(gates)
    weights = [w for pair in zip(gates, ups) for w in pair]
    hidden = (rows // 2, blocks * width)
    outs = [hidden, hidden] + [(rows, depth)] * bool(places)
    return pl.pallas_call(
        lambda *refs: hidden_kernel(places, blocks, *refs),
        out_shape=[jax.ShapeDtypeStruct(out, jnp.bfloat16) for out in outs],
        grid=(1,),
        in_specs=[whole(piece.shape) for piece in pieces]
        + [pl.BlockSpec(memory_space=pltpu.HBM)] * (2 * blocks),
        out_specs=[whole(out) for out in outs],
        scratch_shapes=[
            pltpu.VMEM((blocks, depth, 2 * width), jnp.bfloat16),
            pltpu.SemaphoreType.DMA((2 * blocks,)),
        ],
        compiler_params=pltpu.CompilerParams(vmem_limit_bytes=24 << 20),
        cost_estimate=pl.CostEstimate(
            flops=4 * blocks * rows * depth * width,
            bytes_accessed=2 * (rows * depth + blocks * width * (2 * depth + rows)),
            transcendentals=blocks * rows * width,
        ),
        name="hidden",
    )(*pieces, *weights)


def down_kernel(parts, blocks, *refs):
    hidden_refs, refs = refs[:parts], refs[parts:]
    down_refs, out_refs = refs[:blocks], refs[blocks:]
    width = down_refs[0].shape[0]
    total, block = 0.0, 0
    for hidden_ref in hidden_refs:
        for low in range(0, hidden_ref.shape[1], width):
            total = total + dot(hidden_ref[:, low : low + width], down_refs[block][...])
            block += 1
    height = out_refs[0].shape[0]
    for i, out_ref in enumerate(out_refs):
        out_ref[...] = total[i * height : (i + 1) * height].astype(jnp.bfloat16)


def down_rows(hiddens, downs, pieces):
    rows = hiddens[0].shape[0]
    width, columns = downs[0].shape
    blocks = len(downs)
    depth = blocks * width
    tile = min(columns, 512)
    height = rows // pieces
    return pl.pallas_call(
        lambda *refs: down_kernel(len(hiddens), blocks, *refs),
        out_shape=[jax.ShapeDtypeStruct((height, columns), jnp.bfloat16)] * pieces,
        grid=(columns // tile,),
        in_specs=[whole(hidden.shape) for hidden in hiddens]
        + [pl.BlockSpec((width, tile), lambda i: (0, i))] * blocks,
        out_specs=[pl.BlockSpec((height, tile), lambda i: (0, i))] * pieces,
        compiler_params=pltpu.CompilerParams(vmem_limit_bytes=20 << 20),
        cost_estimate=pl.CostEstimate(
            flops=2 * rows * depth * columns,
            bytes_accessed=2 * (rows * depth + depth * columns + rows * columns),
            transcendentals=0,
        ),
        name="down",
    )(*hiddens, *downs)


def placed_kernel(parts, pick_ref, *refs):
    rows_refs, out_refs = refs[:parts], refs[parts:]
    height = out_refs[0].shape[0]
    low = 0
    for rows_ref in rows_refs:
        high = low + rows_ref.shape[1]
        for i, out_ref in enumerate(out_refs):
            pick = pick_ref[i * height : (i + 1) * height]
            out_ref[:, low:high] = dot(pick, rows_ref[...]).astype(jnp.bfloat16)
        low = high


def placed(pick, parts, pieces):
    count = parts[0].shape[0]
    columns = sum(part.shape[1] for part in parts)
    height = pick.shape[0] // pieces
    return pl.pallas_call(
        lambda *refs: placed_kernel(len(parts), *refs),
        out_shape=[jax.ShapeDtypeStruct((height, columns), jnp.bfloat16)] * pieces,
        grid=(1,),
        in_specs=[whole(value.shape) for value in (pick, *parts)],
        out_specs=[whole((height, columns))] * pieces,
        compiler_params=pltpu.CompilerParams(vmem_limit_bytes=16 << 20),
        cost_estimate=pl.CostEstimate(
            flops=2 * pick.shape[0] * count * columns,
            bytes_accessed=2 * (pick.shape[0] + count) * columns,
            transcendentals=0,
        ),
        name="placed",
    )(pick, *parts)


def across_slots(pick, held):
    return lax.dot_general(pick, held, (((0,), (0,)), ((), ())), preferred_element_type=jnp.float32)


def weighted_kernel(pieces, high_ref, low_ref, *refs):
    block_refs, add_refs, (out_ref, held, added, sems) = refs[:pieces], refs[pieces:-4], refs[-4:]
    height = block_refs[0].shape[0]
    copies = [
        pltpu.make_async_copy(ref, held.at[pl.ds(i * height, height), :], sems.at[i])
        for i, ref in enumerate(block_refs)
    ]
    for i, ref in enumerate(add_refs):
        copies.append(pltpu.make_async_copy(ref, added.at[i], sems.at[pieces + i]))
    for copy in copies:
        copy.start()
    for copy in copies:
        copy.wait()
    total = across_slots(high_ref[...], held[...]) + across_slots(low_ref[...], held[...])
    for i in range(len(add_refs)):
        total = total + added[i].astype(jnp.float32)
    out_ref[...] = total.astype(jnp.bfloat16)


def weighted(gates, blocks, adds=()):
    rows = gates[0].shape[1]
    height, columns = blocks[0].shape
    pieces = len(blocks)
    return pl.pallas_call(
        lambda *refs: weighted_kernel(pieces, *refs),
        out_shape=jax.ShapeDtypeStruct((rows, columns), jnp.bfloat16),
        grid=(1,),
        in_specs=[whole(value.shape) for value in gates]
        + [pl.BlockSpec(memory_space=pltpu.HBM)] * (pieces + len(adds)),
        out_specs=whole((rows, columns)),
        scratch_shapes=[
            pltpu.VMEM((pieces * height, columns), jnp.bfloat16),
            pltpu.VMEM((max(len(adds), 1), rows, columns), jnp.bfloat16),
            pltpu.SemaphoreType.DMA((pieces + len(adds),)),
        ],
        compiler_params=pltpu.CompilerParams(vmem_limit_bytes=16 << 20),
        cost_estimate=pl.CostEstimate(
            flops=4 * pieces * height * rows * columns,
            bytes_accessed=2 * (pieces * height + rows) * columns,
            transcendentals=0,
        ),
        name="weighted",
    )(*gates, *blocks, *adds)


def route_kernel(experts, capacity, where_ref, about_ref, place_ref, high_ref, low_ref):
    low, order = where_ref[0], where_ref[1]
    rows = about_ref.shape[1]
    first = about_ref[0:1, :].astype(jnp.int32) - low
    second = about_ref[1:2, :].astype(jnp.int32) - low
    height = max(experts, 8)
    named = lax.broadcasted_iota(jnp.int32, (height, rows), 0)
    first_hot = (named == first).astype(jnp.float32)
    second_hot = (named == second).astype(jnp.float32)
    down = lax.broadcasted_iota(jnp.int32, (rows, rows), 0)
    right = lax.broadcasted_iota(jnp.int32, (rows, rows), 1)
    earlier = (down < right).astype(jnp.float32).astype(jnp.bfloat16)
    before = dot((first_hot + second_hot).astype(jnp.bfloat16), earlier)
    slot = lax.broadcasted_iota(jnp.int32, (experts * capacity, rows), 0)
    weight, gap = about_ref[2:3, :], about_ref[3:4, :]
    place, gates = 0.0, 0.0
    for ids, hot, gate in (
        (first, first_hot, weight * jax.nn.sigmoid(gap)),
        (second, second_hot, weight * jax.nn.sigmoid(-gap)),
    ):
        rank = jnp.sum(before * hot, axis=0, keepdims=True).astype(jnp.int32)
        here = (ids >= 0) & (ids < experts)
        mine = jnp.where(here, (ids ^ order) * capacity + rank, -1)
        pick = (slot == mine).astype(jnp.float32)
        place = place + pick
        gates = gates + pick * gate
    place_ref[...] = place.astype(jnp.bfloat16)
    high = gates.astype(jnp.bfloat16)
    high_ref[...] = high
    low_ref[...] = (gates - high.astype(jnp.float32)).astype(jnp.bfloat16)


def routing(about, experts, capacity, low, order):
    shape = (experts * capacity, about.shape[1])
    where = jnp.stack([low, order]).astype(jnp.int32)
    return pl.pallas_call(
        lambda *refs: route_kernel(experts, capacity, *refs),
        out_shape=[jax.ShapeDtypeStruct(shape, jnp.bfloat16)] * 3,
        grid_spec=pltpu.PrefetchScalarGridSpec(
            num_scalar_prefetch=1,
            grid=(1,),
            in_specs=[pl.BlockSpec(about.shape, lambda i, where: (0, 0))],
            out_specs=[pl.BlockSpec(shape, lambda i, where: (0, 0))] * 3,
        ),
        compiler_params=pltpu.CompilerParams(vmem_limit_bytes=8 << 20),
        cost_estimate=pl.CostEstimate(
            flops=40 * shape[0] * shape[1], bytes_accessed=6 * shape[0] * shape[1], transcendentals=0
        ),
        name="route",
    )(where, about)


def conv_kernel(blocks, taps, halo, *refs):
    window_refs, small_refs, refs = refs[:blocks], refs[blocks : 2 * blocks], refs[2 * blocks :]
    out_ref, gains_ref, wide, held = refs
    rows, width = out_ref.shape[0], window_refs[0].shape[1]
    row_sum, row_sq = 0.0, 0.0
    for block in range(blocks):
        wide[...] = window_refs[block][...].astype(jnp.float32)
        total = jnp.zeros((rows, width), jnp.float32)
        for tap in range(taps):
            start = halo - taps + 1 + tap
            total = total + small_refs[block][tap : tap + 1, :] * wide[start : start + rows, :]
        held[block] = total
        row_sum = row_sum + jnp.sum(total, axis=-1, keepdims=True)
        row_sq = row_sq + jnp.sum(total * total, axis=-1, keepdims=True)
        gains = small_refs[block][taps + 2 :, :]
        gains_ref[block * gains.shape[0] : (block + 1) * gains.shape[0], :] = gains
    mean = row_sum / CH
    scale = lax.rsqrt(row_sq / CH - mean * mean + eps)
    for block in range(blocks):
        gain, shift = small_refs[block][taps : taps + 1, :], small_refs[block][taps + 1 : taps + 2, :]
        normalized = (held[block] - mean) * scale * gain + shift
        out_ref[:, block * width : (block + 1) * width] = jax.nn.silu(normalized).astype(jnp.bfloat16)


def conv_rows(windows, smalls, taps):
    high, width = windows[0].shape
    halo = -(-(taps - 1) // 16) * 16
    rows, blocks = high - halo, len(windows)
    gains = (blocks * (smalls[0].shape[0] - taps - 2), width)
    return pl.pallas_call(
        lambda *refs: conv_kernel(blocks, taps, halo, *refs),
        out_shape=[
            jax.ShapeDtypeStruct((rows, blocks * width), jnp.bfloat16),
            jax.ShapeDtypeStruct(gains, jnp.float32),
        ],
        grid=(1,),
        in_specs=[whole(value.shape) for value in (*windows, *smalls)],
        out_specs=[whole((rows, blocks * width)), whole(gains)],
        scratch_shapes=[
            pltpu.VMEM((high, width), jnp.float32),
            pltpu.VMEM((blocks, rows, width), jnp.float32),
        ],
        compiler_params=pltpu.CompilerParams(vmem_limit_bytes=16 << 20),
        cost_estimate=pl.CostEstimate(
            flops=2 * taps * rows * blocks * width,
            bytes_accessed=4 * blocks * high * width,
            transcendentals=blocks * rows * width,
        ),
        name="conv",
    )(*windows, *smalls)


def near_kernel(blocks, act_ref, *refs):
    weight_refs, out_ref = refs[:blocks], refs[blocks]
    width = weight_refs[0].shape[0]
    total = 0.0
    for block, ref in enumerate(weight_refs):
        total = total + dot(act_ref[:, block * width : (block + 1) * width], ref[...])
    out_ref[...] = total


def near_product(act, weights):
    rows = act.shape[0]
    width, columns = weights[0].shape
    tile = min(columns, 1024)
    return pl.pallas_call(
        lambda *refs: near_kernel(len(weights), *refs),
        out_shape=jax.ShapeDtypeStruct((rows, columns), jnp.float32),
        grid=(columns // tile,),
        in_specs=[whole(act.shape)] + [pl.BlockSpec((width, tile), lambda i: (0, i))] * len(weights),
        out_specs=pl.BlockSpec((rows, tile), lambda i: (0, i)),
        compiler_params=pltpu.CompilerParams(vmem_limit_bytes=16 << 20),
        cost_estimate=pl.CostEstimate(
            flops=2 * rows * width * columns * len(weights),
            bytes_accessed=2 * width * columns * len(weights),
            transcendentals=0,
        ),
        name="near_product",
    )(act, *weights)


def middle_kernel(blocks, first, share, where_ref, act_ref, near_ref, gains_ref, *refs):
    count = share * (blocks - first)
    part_refs, residual_refs, refs = refs[:count], refs[count : count + blocks], refs[count + blocks :]
    middle_refs, normed_refs, (total, held, gains, sems) = refs[:2], refs[2:4], refs[4:]
    tp, share_at = where_ref[0], where_ref[1]
    part, columns = part_refs[0].shape
    width = share * part
    copies = []
    for i, ref in enumerate(part_refs):
        row = pl.multiple_of(i // share * width + (share_at ^ (i % share)) * part, part)
        copies.append(pltpu.make_async_copy(ref, held.at[pl.ds(row, part), :], sems.at[i]))
    for copy in copies:
        copy.start()
    for block in range(blocks - first):
        for copy in copies[block * share : (block + 1) * share]:
            copy.wait()
        low = (first + block) * width
        product = dot(act_ref[:, low : low + width], held[block * width : (block + 1) * width])
        total[...] = (total if block else near_ref)[...] + product
    narrow = middle_refs[0].shape[1] // blocks
    row_sq = 0.0
    for block in range(blocks):
        at = tp ^ block
        for k in (0, 1):
            here = pl.ds(pl.multiple_of((2 * at + k) * narrow, narrow), narrow)
            there = pl.ds(pl.multiple_of(at * narrow, narrow), narrow)
            wide = residual_refs[block][:, k * narrow : (k + 1) * narrow].astype(jnp.float32)
            rounded = (wide + total[:, here]).astype(jnp.bfloat16)
            middle_refs[k][:, there] = rounded
            wide = rounded.astype(jnp.float32)
            total[:, here] = wide
            row_sq = row_sq + jnp.sum(wide * wide, axis=-1, keepdims=True)
            for g in range(0, narrow, width):
                line = (2 * block + k) * narrow // width + g // width
                lane = pl.multiple_of((2 * at + k) * narrow + g, width)
                gains[:, pl.ds(lane, width)] = gains_ref[line : line + 1, :]
    scale = lax.rsqrt(row_sq / D + eps)
    half = columns // 2
    for i, ref in enumerate(normed_refs):
        here = slice(i * half, (i + 1) * half)
        ref[...] = (total[:, here] * scale * gains[:, here]).astype(jnp.bfloat16)


def middle_rows(act, near, gains, far_blocks, residuals, where):
    rows, columns = near.shape
    blocks = len(residuals)
    first = blocks - len(far_blocks)
    share = len(far_blocks[0])
    parts = [piece for block in far_blocks for piece in block]
    part = parts[0].shape[0]
    half = (rows, columns // 2)
    spec = lambda shape: pl.BlockSpec(shape, lambda i, where: (0,) * len(shape))
    ins = [act, near, gains]
    return pl.pallas_call(
        lambda *refs: middle_kernel(blocks, first, share, *refs),
        out_shape=[jax.ShapeDtypeStruct(half, jnp.bfloat16)] * 4,
        grid_spec=pltpu.PrefetchScalarGridSpec(
            num_scalar_prefetch=1,
            grid=(1,),
            in_specs=[spec(v.shape) for v in ins]
            + [pl.BlockSpec(memory_space=pl.ANY)] * len(parts)
            + [spec(v.shape) for v in residuals],
            out_specs=[spec(half)] * 4,
            scratch_shapes=[
                pltpu.VMEM((rows, columns), jnp.float32),
                pltpu.VMEM((len(parts) * part, columns), jnp.bfloat16),
                pltpu.VMEM((1, columns), jnp.float32),
                pltpu.SemaphoreType.DMA((len(parts),)),
            ],
        ),
        compiler_params=pltpu.CompilerParams(vmem_limit_bytes=16 << 20),
        cost_estimate=pl.CostEstimate(
            flops=2 * rows * len(parts) * part * columns,
            bytes_accessed=2 * len(parts) * part * columns,
            transcendentals=0,
        ),
        name="middle",
    )(where, *ins, *parts, *residuals)


def shards(
    conv_value,
    conv_gate,
    conv_weight,
    conv_gain,
    conv_shift,
    out_weight,
    residual,
    mix_gain,
    expert_ids,
    group_weight,
    score_gap,
    w_gate,
    w_up,
    w_down,
):
    row_count, width = conv_value.shape
    taps = conv_weight.shape[0]
    reach = taps - 1
    halo = -(-reach // 16) * 16
    seq_devices = lax.axis_size(("h", "r"))
    half_devices = lax.axis_size("r")
    tp_devices = lax.axis_size("tp")
    far = tp_devices // 2
    quarter = row_count // tp_devices
    capacity = 4 * quarter // seq_devices
    col_count = residual.shape[1]
    tp = lax.axis_index("tp")
    half = lax.axis_index("h")
    share = min(4, half_devices)
    share_at = lax.axis_index("r") % share
    part = width // share

    def mine(value, axis=0):
        return lax.dynamic_slice_in_dim(value, tp * quarter, quarter, axis)

    part_own = swap(lax.dynamic_slice_in_dim(out_weight, share_at * part, part, 0), far)
    parts = [part_own]
    for bit in range(1, share):
        pairs = [(i, i ^ bit) for i in range(half_devices)]
        parts.append(lax.ppermute(part_own, "r", pairs))
    out_blocks = {0: out_weight, far: parts}
    bit = far // 2
    while bit:
        for have in sorted(out_blocks):
            if have < far:
                out_blocks[bit ^ have] = swap(out_blocks[have], bit)
            else:
                pieces = []
                for piece in out_blocks[have]:
                    pieces.append(swap(piece, bit))
                out_blocks[bit ^ have] = pieces
        bit //= 2

    small = jnp.concatenate(
        [conv_weight, conv_gain[None], conv_shift[None], mix_gain.reshape(-1, width)], axis=0
    )
    gated = conv_value.astype(jnp.float32) * jax.nn.sigmoid(conv_gate.astype(jnp.float32))
    gated = gated.astype(jnp.bfloat16)
    previous = lax.ppermute(
        gated[row_count - halo :], ("h", "r"), [(i, i + 1) for i in range(seq_devices - 1)]
    )
    padded = jnp.concatenate([previous, gated], axis=0)
    windows = exchanged(
        lambda bit: lax.dynamic_slice_in_dim(padded, (tp ^ bit) * quarter, halo + quarter, 0),
    )
    smalls = exchanged(lambda bit: small)
    windows[1], w_down = lax.optimization_barrier((windows[1], w_down))
    residuals = exchanged(
        lambda bit: lax.dynamic_slice_in_dim(residual, (tp ^ bit) * quarter, quarter, 0),
    )
    gates = gathered(w_gate[0])
    ups = gathered(w_up[0])
    narrow = col_count // 2

    def columns(value, k):
        return jnp.concatenate(
            [value[:, low : low + narrow] for low in range(k * narrow, D, col_count)], axis=1
        )

    own_downs = [columns(w_down[0], k) for k in (0, 1)]
    downs = [gathered(own_downs[k]) for k in (0, 1)]

    own_about = jnp.concatenate(
        [
            mine(expert_ids.T, 1).astype(jnp.float32),
            mine(group_weight[None], 1),
            mine(score_gap[None], 1),
        ]
    )
    other_about = lax.ppermute(own_about, "h", [(0, 1), (1, 0)])
    order = lax.axis_index("r") if half_devices <= FEW else jnp.int32(0)
    low = half * half_devices
    own_place, *own_gates = routing(own_about, half_devices, capacity, low, order)
    other_place, *other_gates = routing(other_about, half_devices, capacity, low, order)

    act, gains = conv_rows(windows, smalls, taps)
    near = near_product(act, [out_blocks[bit] for bit in range(far)])
    far_blocks = [out_blocks[bit] for bit in range(far, tp_devices)]
    *middle, normed_low, normed_high = middle_rows(
        act, near, gains, far_blocks, residuals, jnp.stack([tp, share_at]).astype(jnp.int32)
    )
    normed = [normed_low, normed_high]

    def inside(blocks):
        if half_devices <= FEW:
            got = [blocks[0]]
            for bit in range(1, half_devices):
                pairs = [(i, i ^ bit) for i in range(half_devices)]
                got.append(lax.ppermute(blocks[bit], "r", pairs))
            return got
        got = lax.all_to_all(
            blocks[0].reshape(half_devices, capacity, -1), "r", 0, 0, tiled=True
        )
        return [got.reshape(half_devices * capacity, -1)]

    def crossed(rows):
        return lax.ppermute(rows, "h", [(0, 1), (1, 0)])

    pieces = half_devices if half_devices <= FEW else 1
    other_parts = [crossed(rows) for rows in normed]
    own_in = inside(placed(own_place, normed, pieces))
    other_in = [inside(placed(other_place, [rows], pieces)) for rows in other_parts]
    places, tops = [], [0, half_devices * capacity]
    for top, parts in zip(tops, ([own_in], other_in)):
        left = 0
        for part in parts:
            places += [(top + i * part[0].shape[0], left) for i in range(len(part))]
            left += part[0].shape[1]
    x_pieces = [block for part in [own_in] + other_in for block in part]
    rows = 2 * half_devices * capacity
    near_own, near_other, x = hidden_rows(x_pieces, places, rows, gates[:far], ups[:far])
    far_own, far_other = hidden_rows([x], [], rows, gates[far:], ups[far:])
    own_hidden, other_hidden = [near_own, far_own], [near_other, far_other]

    outputs = []
    for k in (0, 1):
        across = inside(down_rows(other_hidden, downs[k], pieces))
        back = crossed(weighted(other_gates, across))
        within = inside(down_rows(own_hidden, downs[k], pieces))
        result = weighted(own_gates, within, (middle[k], back))
        rows = natural(
            exchanged(lambda bit: lax.dynamic_slice_in_dim(result, (tp ^ bit) * narrow, narrow, 1)),
            tp,
        )
        outputs.append(jnp.concatenate(rows, axis=0))
    return jnp.concatenate(outputs, axis=1)


def solution(mesh):
    count = mesh.shape["sp"]
    split = Mesh(mesh.devices.reshape(2, count // 2, -1), ("h", "r", "tp"))
    sp = ("h", "r")
    return jax.shard_map(
        shards,
        mesh=split,
        in_specs=(
            P(sp, "tp"),
            P(sp, "tp"),
            P(None, "tp"),
            P("tp"),
            P("tp"),
            P("tp", None),
            P(sp, "tp"),
            P("tp"),
            P(sp, None),
            P(sp),
            P(sp),
            P(sp, None, "tp"),
            P(sp, None, "tp"),
            P(sp, "tp", None),
        ),
        out_specs=P(sp, "tp"),
        check_vma=False,
    )
```

```python
import jax
import jax.numpy as jnp
from jax import lax
from jax.experimental import pallas as pl
from jax.experimental.pallas import tpu as pltpu
from jax.sharding import Mesh
from jax.sharding import PartitionSpec as P


D = 2048
CH = 1024


eps = 1e-06
FEW = 8


def swap(value, bit):
    count = lax.axis_size("tp")
    return lax.ppermute(value, "tp", [(source, source ^ bit) for source in range(count)])


def natural(blocks, index):
    ordered = []
    for place in range(len(blocks)):
        chosen = blocks[0]
        for bit in range(1, len(blocks)):
            chosen = jnp.where(index == (place ^ bit), blocks[bit], chosen)
        ordered.append(chosen)
    return ordered


def exchanged(piece):
    count = lax.axis_size("tp")
    blocks = [piece(0)]
    for bit in range(1, count):
        blocks.append(swap(piece(bit), bit))
    return blocks


def gathered(block):
    count = lax.axis_size("tp")
    held = {0: block}
    bit = count // 2
    while bit:
        for have in sorted(held):
            held[bit ^ have] = swap(held[have], bit)
        bit //= 2
    return [held[bit] for bit in range(count)]


def dot(left, right):
    return jnp.dot(left, right, preferred_element_type=jnp.float32)


def hidden_kernel(places, blocks, *refs):
    pieces = max(len(places), 1)
    x_refs, refs = refs[:pieces], refs[pieces:]
    weight_refs, refs = refs[: 2 * blocks], refs[2 * blocks :]
    own_ref, other_ref, refs = refs[0], refs[1], refs[2:]
    x, (held, sems) = (refs[0], refs[1:]) if places else (x_refs[0], refs)
    width = weight_refs[0].shape[1]
    copies = [
        pltpu.make_async_copy(ref, held.at[i // 2, :, pl.ds(i % 2 * width, width)], sems.at[i])
        for i, ref in enumerate(weight_refs)
    ]
    for copy in copies:
        copy.start()
    for (top, left), x_ref in zip(places, x_refs):
        height, columns = x_ref.shape
        x[top : top + height, left : left + columns] = x_ref[...]
    half = own_ref.shape[0]
    for block in range(blocks):
        copies[2 * block].wait()
        copies[2 * block + 1].wait()
        for i, out_ref in enumerate((own_ref, other_ref)):
            both = dot(x[i * half : (i + 1) * half], held[block])
            gate, up = both[:, :width], both[:, width:]
            out_ref[:, block * width : (block + 1) * width] = (jax.nn.silu(gate) * up).astype(
                jnp.bfloat16
            )


def whole(shape):
    return pl.BlockSpec(shape, lambda i: (0,) * len(shape))


def hidden_rows(pieces, places, rows, gates, ups):
    depth, width = gates[0].shape
    blocks = len(gates)
    weights = [w for pair in zip(gates, ups) for w in pair]
    hidden = (rows // 2, blocks * width)
    outs = [hidden, hidden] + [(rows, depth)] * bool(places)
    return pl.pallas_call(
        lambda *refs: hidden_kernel(places, blocks, *refs),
        out_shape=[jax.ShapeDtypeStruct(out, jnp.bfloat16) for out in outs],
        grid=(1,),
        in_specs=[whole(piece.shape) for piece in pieces]
        + [pl.BlockSpec(memory_space=pltpu.HBM)] * (2 * blocks),
        out_specs=[whole(out) for out in outs],
        scratch_shapes=[
            pltpu.VMEM((blocks, depth, 2 * width), jnp.bfloat16),
            pltpu.SemaphoreType.DMA((2 * blocks,)),
        ],
        compiler_params=pltpu.CompilerParams(vmem_limit_bytes=24 << 20),
        cost_estimate=pl.CostEstimate(
            flops=4 * blocks * rows * depth * width,
            bytes_accessed=2 * (rows * depth + blocks * width * (2 * depth + rows)),
            transcendentals=blocks * rows * width,
        ),
        name="hid",
    )(*pieces, *weights)


def down_kernel(parts, blocks, *refs):
    hidden_refs, refs = refs[:parts], refs[parts:]
    down_refs, out_refs = refs[:blocks], refs[blocks:]
    width = down_refs[0].shape[0]
    total, block = 0.0, 0
    for hidden_ref in hidden_refs:
        for low in range(0, hidden_ref.shape[1], width):
            total = total + dot(hidden_ref[:, low : low + width], down_refs[block][...])
            block += 1
    height = out_refs[0].shape[0]
    for i, out_ref in enumerate(out_refs):
        out_ref[...] = total[i * height : (i + 1) * height].astype(jnp.bfloat16)


def down_rows(hiddens, downs, pieces):
    rows = hiddens[0].shape[0]
    width, columns = downs[0].shape
    blocks = len(downs)
    depth = blocks * width
    tile = min(columns, 512)
    height = rows // pieces
    return pl.pallas_call(
        lambda *refs: down_kernel(len(hiddens), blocks, *refs),
        out_shape=[jax.ShapeDtypeStruct((height, columns), jnp.bfloat16)] * pieces,
        grid=(columns // tile,),
        in_specs=[whole(hidden.shape) for hidden in hiddens]
        + [pl.BlockSpec((width, tile), lambda i: (0, i))] * blocks,
        out_specs=[pl.BlockSpec((height, tile), lambda i: (0, i))] * pieces,
        compiler_params=pltpu.CompilerParams(vmem_limit_bytes=20 << 20),
        cost_estimate=pl.CostEstimate(
            flops=2 * rows * depth * columns,
            bytes_accessed=2 * (rows * depth + depth * columns + rows * columns),
            transcendentals=0,
        ),
        name="down",
    )(*hiddens, *downs)


def placed_kernel(parts, pick_ref, *refs):
    rows_refs, out_refs = refs[:parts], refs[parts:]
    height = out_refs[0].shape[0]
    low = 0
    for rows_ref in rows_refs:
        high = low + rows_ref.shape[1]
        for i, out_ref in enumerate(out_refs):
            pick = pick_ref[i * height : (i + 1) * height]
            out_ref[:, low:high] = dot(pick, rows_ref[...]).astype(jnp.bfloat16)
        low = high


def placed(pick, parts, pieces):
    count = parts[0].shape[0]
    columns = sum(part.shape[1] for part in parts)
    height = pick.shape[0] // pieces
    return pl.pallas_call(
        lambda *refs: placed_kernel(len(parts), *refs),
        out_shape=[jax.ShapeDtypeStruct((height, columns), jnp.bfloat16)] * pieces,
        grid=(1,),
        in_specs=[whole(value.shape) for value in (pick, *parts)],
        out_specs=[whole((height, columns))] * pieces,
        compiler_params=pltpu.CompilerParams(vmem_limit_bytes=16 << 20),
        cost_estimate=pl.CostEstimate(
            flops=2 * pick.shape[0] * count * columns,
            bytes_accessed=2 * (pick.shape[0] + count) * columns,
            transcendentals=0,
        ),
        name="placed",
    )(pick, *parts)


def across_slots(pick, held):
    return lax.dot_general(pick, held, (((0,), (0,)), ((), ())), preferred_element_type=jnp.float32)


def weighted_kernel(pieces, high_ref, low_ref, *refs):
    block_refs, add_refs, (out_ref, held, added, sems) = refs[:pieces], refs[pieces:-4], refs[-4:]
    height = block_refs[0].shape[0]
    copies = [
        pltpu.make_async_copy(ref, held.at[pl.ds(i * height, height), :], sems.at[i])
        for i, ref in enumerate(block_refs)
    ]
    for i, ref in enumerate(add_refs):
        copies.append(pltpu.make_async_copy(ref, added.at[i], sems.at[pieces + i]))
    for copy in copies:
        copy.start()
    for copy in copies:
        copy.wait()
    total = across_slots(high_ref[...], held[...]) + across_slots(low_ref[...], held[...])
    for i in range(len(add_refs)):
        total = total + added[i].astype(jnp.float32)
    out_ref[...] = total.astype(jnp.bfloat16)


def weighted(gates, blocks, adds=()):
    rows = gates[0].shape[1]
    height, columns = blocks[0].shape
    pieces = len(blocks)
    return pl.pallas_call(
        lambda *refs: weighted_kernel(pieces, *refs),
        out_shape=jax.ShapeDtypeStruct((rows, columns), jnp.bfloat16),
        grid=(1,),
        in_specs=[whole(value.shape) for value in gates]
        + [pl.BlockSpec(memory_space=pltpu.HBM)] * (pieces + len(adds)),
        out_specs=whole((rows, columns)),
        scratch_shapes=[
            pltpu.VMEM((pieces * height, columns), jnp.bfloat16),
            pltpu.VMEM((max(len(adds), 1), rows, columns), jnp.bfloat16),
            pltpu.SemaphoreType.DMA((pieces + len(adds),)),
        ],
        compiler_params=pltpu.CompilerParams(vmem_limit_bytes=16 << 20),
        cost_estimate=pl.CostEstimate(
            flops=4 * pieces * height * rows * columns,
            bytes_accessed=2 * (pieces * height + rows) * columns,
            transcendentals=0,
        ),
        name="weighted",
    )(*gates, *blocks, *adds)


def route_kernel(experts, capacity, where_ref, about_ref, place_ref, high_ref, low_ref):
    low, order = where_ref[0], where_ref[1]
    rows = about_ref.shape[1]
    first = about_ref[0:1, :].astype(jnp.int32) - low
    second = about_ref[1:2, :].astype(jnp.int32) - low
    height = max(experts, 8)
    named = lax.broadcasted_iota(jnp.int32, (height, rows), 0)
    first_hot = (named == first).astype(jnp.float32)
    second_hot = (named == second).astype(jnp.float32)
    down = lax.broadcasted_iota(jnp.int32, (rows, rows), 0)
    right = lax.broadcasted_iota(jnp.int32, (rows, rows), 1)
    earlier = (down < right).astype(jnp.float32).astype(jnp.bfloat16)
    before = dot((first_hot + second_hot).astype(jnp.bfloat16), earlier)
    slot = lax.broadcasted_iota(jnp.int32, (experts * capacity, rows), 0)
    weight, gap = about_ref[2:3, :], about_ref[3:4, :]
    place, gates = 0.0, 0.0
    for ids, hot, gate in (
        (first, first_hot, weight * jax.nn.sigmoid(gap)),
        (second, second_hot, weight * jax.nn.sigmoid(-gap)),
    ):
        rank = jnp.sum(before * hot, axis=0, keepdims=True).astype(jnp.int32)
        here = (ids >= 0) & (ids < experts)
        mine = jnp.where(here, (ids ^ order) * capacity + rank, -1)
        pick = (slot == mine).astype(jnp.float32)
        place = place + pick
        gates = gates + pick * gate
    place_ref[...] = place.astype(jnp.bfloat16)
    high = gates.astype(jnp.bfloat16)
    high_ref[...] = high
    low_ref[...] = (gates - high.astype(jnp.float32)).astype(jnp.bfloat16)


def routing(about, experts, capacity, low, order):
    shape = (experts * capacity, about.shape[1])
    where = jnp.stack([low, order]).astype(jnp.int32)
    return pl.pallas_call(
        lambda *refs: route_kernel(experts, capacity, *refs),
        out_shape=[jax.ShapeDtypeStruct(shape, jnp.bfloat16)] * 3,
        grid_spec=pltpu.PrefetchScalarGridSpec(
            num_scalar_prefetch=1,
            grid=(1,),
            in_specs=[pl.BlockSpec(about.shape, lambda i, where: (0, 0))],
            out_specs=[pl.BlockSpec(shape, lambda i, where: (0, 0))] * 3,
        ),
        compiler_params=pltpu.CompilerParams(vmem_limit_bytes=8 << 20),
        cost_estimate=pl.CostEstimate(
            flops=40 * shape[0] * shape[1], bytes_accessed=6 * shape[0] * shape[1], transcendentals=0
        ),
        name="route",
    )(where, about)


def conv_kernel(blocks, taps, halo, *refs):
    window_refs, small_refs, refs = refs[:blocks], refs[blocks : 2 * blocks], refs[2 * blocks :]
    out_ref, gains_ref, wide, held = refs
    rows, width = out_ref.shape[0], window_refs[0].shape[1]
    row_sum, row_sq = 0.0, 0.0
    for block in range(blocks):
        wide[...] = window_refs[block][...].astype(jnp.float32)
        total = jnp.zeros((rows, width), jnp.float32)
        for tap in range(taps):
            start = halo - taps + 1 + tap
            total = total + small_refs[block][tap : tap + 1, :] * wide[start : start + rows, :]
        held[block] = total
        row_sum = row_sum + jnp.sum(total, axis=-1, keepdims=True)
        row_sq = row_sq + jnp.sum(total * total, axis=-1, keepdims=True)
        gains = small_refs[block][taps + 2 :, :]
        gains_ref[block * gains.shape[0] : (block + 1) * gains.shape[0], :] = gains
    mean = row_sum / CH
    scale = lax.rsqrt(row_sq / CH - mean * mean + eps)
    for block in range(blocks):
        gain, shift = small_refs[block][taps : taps + 1, :], small_refs[block][taps + 1 : taps + 2, :]
        normalized = (held[block] - mean) * scale * gain + shift
        out_ref[:, block * width : (block + 1) * width] = jax.nn.silu(normalized).astype(jnp.bfloat16)


def conv_rows(windows, smalls, taps):
    high, width = windows[0].shape
    halo = -(-(taps - 1) // 16) * 16
    rows, blocks = high - halo, len(windows)
    gains = (blocks * (smalls[0].shape[0] - taps - 2), width)
    return pl.pallas_call(
        lambda *refs: conv_kernel(blocks, taps, halo, *refs),
        out_shape=[
            jax.ShapeDtypeStruct((rows, blocks * width), jnp.bfloat16),
            jax.ShapeDtypeStruct(gains, jnp.float32),
        ],
        grid=(1,),
        in_specs=[whole(value.shape) for value in (*windows, *smalls)],
        out_specs=[whole((rows, blocks * width)), whole(gains)],
        scratch_shapes=[
            pltpu.VMEM((high, width), jnp.float32),
            pltpu.VMEM((blocks, rows, width), jnp.float32),
        ],
        compiler_params=pltpu.CompilerParams(vmem_limit_bytes=16 << 20),
        cost_estimate=pl.CostEstimate(
            flops=2 * taps * rows * blocks * width,
            bytes_accessed=4 * blocks * high * width,
            transcendentals=blocks * rows * width,
        ),
        name="conv",
    )(*windows, *smalls)


def near_kernel(blocks, act_ref, *refs):
    weight_refs, out_ref = refs[:blocks], refs[blocks]
    width = weight_refs[0].shape[0]
    total = 0.0
    for block, ref in enumerate(weight_refs):
        total = total + dot(act_ref[:, block * width : (block + 1) * width], ref[...])
    out_ref[...] = total


def near_product(act, weights):
    rows = act.shape[0]
    width, columns = weights[0].shape
    tile = min(columns, 1024)
    return pl.pallas_call(
        lambda *refs: near_kernel(len(weights), *refs),
        out_shape=jax.ShapeDtypeStruct((rows, columns), jnp.float32),
        grid=(columns // tile,),
        in_specs=[whole(act.shape)] + [pl.BlockSpec((width, tile), lambda i: (0, i))] * len(weights),
        out_specs=pl.BlockSpec((rows, tile), lambda i: (0, i), memory_space=pltpu.VMEM),
        compiler_params=pltpu.CompilerParams(vmem_limit_bytes=16 << 20),
        cost_estimate=pl.CostEstimate(
            flops=2 * rows * width * columns * len(weights),
            bytes_accessed=2 * width * columns * len(weights),
            transcendentals=0,
        ),
        name="near",
    )(act, *weights)


def middle_kernel(blocks, first, share, where_ref, act_ref, near_ref, gains_ref, *refs):
    count = share * (blocks - first)
    part_refs, residual_refs, refs = refs[:count], refs[count : count + blocks], refs[count + blocks :]
    middle_refs, normed_refs, (total, held, gains, sems) = refs[:2], refs[2:4], refs[4:]
    tp, share_at = where_ref[0], where_ref[1]
    part, columns = part_refs[0].shape
    width = share * part
    copies = []
    for i, ref in enumerate(part_refs):
        row = pl.multiple_of(i // share * width + (share_at ^ (i % share)) * part, part)
        copies.append(pltpu.make_async_copy(ref, held.at[pl.ds(row, part), :], sems.at[i]))
    for copy in copies:
        copy.start()
    for block in range(blocks - first):
        for copy in copies[block * share : (block + 1) * share]:
            copy.wait()
        low = (first + block) * width
        product = dot(act_ref[:, low : low + width], held[block * width : (block + 1) * width])
        total[...] = (total if block else near_ref)[...] + product
    narrow = middle_refs[0].shape[1] // blocks
    row_sq = 0.0
    for block in range(blocks):
        at = tp ^ block
        for k in (0, 1):
            here = pl.ds(pl.multiple_of((2 * at + k) * narrow, narrow), narrow)
            there = pl.ds(pl.multiple_of(at * narrow, narrow), narrow)
            wide = residual_refs[block][:, k * narrow : (k + 1) * narrow].astype(jnp.float32)
            rounded = (wide + total[:, here]).astype(jnp.bfloat16)
            middle_refs[k][:, there] = rounded
            wide = rounded.astype(jnp.float32)
            total[:, here] = wide
            row_sq = row_sq + jnp.sum(wide * wide, axis=-1, keepdims=True)
            for g in range(0, narrow, width):
                line = (2 * block + k) * narrow // width + g // width
                lane = pl.multiple_of((2 * at + k) * narrow + g, width)
                gains[:, pl.ds(lane, width)] = gains_ref[line : line + 1, :]
    scale = lax.rsqrt(row_sq / D + eps)
    half = columns // 2
    for i, ref in enumerate(normed_refs):
        here = slice(i * half, (i + 1) * half)
        ref[...] = (total[:, here] * scale * gains[:, here]).astype(jnp.bfloat16)


def middle_rows(act, near, gains, far_blocks, residuals, where):
    rows, columns = near.shape
    blocks = len(residuals)
    first = blocks - len(far_blocks)
    share = len(far_blocks[0])
    parts = [piece for block in far_blocks for piece in block]
    part = parts[0].shape[0]
    half = (rows, columns // 2)
    spec = lambda shape: pl.BlockSpec(shape, lambda i, where: (0,) * len(shape))
    ins = [act, near, gains]
    return pl.pallas_call(
        lambda *refs: middle_kernel(blocks, first, share, *refs),
        out_shape=[jax.ShapeDtypeStruct(half, jnp.bfloat16)] * 4,
        grid_spec=pltpu.PrefetchScalarGridSpec(
            num_scalar_prefetch=1,
            grid=(1,),
            in_specs=[pl.BlockSpec(memory_space=pltpu.VMEM)] * len(ins)
            + [pl.BlockSpec(memory_space=pl.ANY)] * len(parts)
            + [spec(v.shape) for v in residuals],
            out_specs=[spec(half)] * 4,
            scratch_shapes=[
                pltpu.VMEM((rows, columns), jnp.float32),
                pltpu.VMEM((len(parts) * part, columns), jnp.bfloat16),
                pltpu.VMEM((1, columns), jnp.float32),
                pltpu.SemaphoreType.DMA((len(parts),)),
            ],
        ),
        compiler_params=pltpu.CompilerParams(vmem_limit_bytes=16 << 20),
        cost_estimate=pl.CostEstimate(
            flops=2 * rows * len(parts) * part * columns,
            bytes_accessed=2 * len(parts) * part * columns,
            transcendentals=0,
        ),
        name="middle",
    )(where, *ins, *parts, *residuals)


def shards(
    conv_value,
    conv_gate,
    conv_weight,
    conv_gain,
    conv_shift,
    out_weight,
    residual,
    mix_gain,
    expert_ids,
    group_weight,
    score_gap,
    w_gate,
    w_up,
    w_down,
):
    row_count, width = conv_value.shape
    taps = conv_weight.shape[0]
    reach = taps - 1
    halo = -(-reach // 16) * 16
    seq_devices = lax.axis_size(("h", "r"))
    half_devices = lax.axis_size("r")
    tp_devices = lax.axis_size("tp")
    far = tp_devices // 2
    quarter = row_count // tp_devices
    capacity = 4 * quarter // seq_devices
    col_count = residual.shape[1]
    tp = lax.axis_index("tp")
    half = lax.axis_index("h")
    share = min(4, half_devices)
    share_at = lax.axis_index("r") % share
    part = width // share

    def mine(value, axis=0):
        return lax.dynamic_slice_in_dim(value, tp * quarter, quarter, axis)

    part_own = swap(lax.dynamic_slice_in_dim(out_weight, share_at * part, part, 0), far)
    parts = [part_own]
    for bit in range(1, share):
        pairs = [(i, i ^ bit) for i in range(half_devices)]
        parts.append(lax.ppermute(part_own, "r", pairs))
    out_blocks = {0: out_weight, far: parts}
    bit = far // 2
    while bit:
        for have in sorted(out_blocks):
            if have < far:
                out_blocks[bit ^ have] = swap(out_blocks[have], bit)
            else:
                pieces = []
                for piece in out_blocks[have]:
                    pieces.append(swap(piece, bit))
                out_blocks[bit ^ have] = pieces
        bit //= 2

    small = jnp.concatenate(
        [conv_weight, conv_gain[None], conv_shift[None], mix_gain.reshape(-1, width)], axis=0
    )
    gated = conv_value.astype(jnp.float32) * jax.nn.sigmoid(conv_gate.astype(jnp.float32))
    gated = gated.astype(jnp.bfloat16)
    previous = lax.ppermute(
        gated[row_count - halo :], ("h", "r"), [(i, i + 1) for i in range(seq_devices - 1)]
    )
    padded = jnp.concatenate([previous, gated], axis=0)
    windows = exchanged(
        lambda bit: lax.dynamic_slice_in_dim(padded, (tp ^ bit) * quarter, halo + quarter, 0),
    )
    smalls = exchanged(lambda bit: small)
    windows[1], w_down = lax.optimization_barrier((windows[1], w_down))
    residuals = exchanged(
        lambda bit: lax.dynamic_slice_in_dim(residual, (tp ^ bit) * quarter, quarter, 0),
    )
    gates = gathered(w_gate[0])
    ups = gathered(w_up[0])
    narrow = col_count // 2

    def columns(value, k):
        return jnp.concatenate(
            [value[:, low : low + narrow] for low in range(k * narrow, D, col_count)], axis=1
        )

    own_downs = [columns(w_down[0], k) for k in (0, 1)]
    downs = [gathered(own_downs[k]) for k in (0, 1)]

    own_about = jnp.concatenate(
        [
            mine(expert_ids.T, 1).astype(jnp.float32),
            mine(group_weight[None], 1),
            mine(score_gap[None], 1),
        ]
    )
    other_about = lax.ppermute(own_about, "h", [(0, 1), (1, 0)])
    order = lax.axis_index("r") if half_devices <= FEW else jnp.int32(0)
    low = half * half_devices
    own_place, *own_gates = routing(own_about, half_devices, capacity, low, order)
    other_place, *other_gates = routing(other_about, half_devices, capacity, low, order)

    act, gains = conv_rows(windows, smalls, taps)
    near = near_product(act, [out_blocks[bit] for bit in range(far)])
    far_blocks = [out_blocks[bit] for bit in range(far, tp_devices)]
    *middle, normed_low, normed_high = middle_rows(
        act, near, gains, far_blocks, residuals, jnp.stack([tp, share_at]).astype(jnp.int32)
    )
    normed = [normed_low, normed_high]

    def inside(blocks):
        if half_devices <= FEW:
            got = [blocks[0]]
            for bit in range(1, half_devices):
                pairs = [(i, i ^ bit) for i in range(half_devices)]
                got.append(lax.ppermute(blocks[bit], "r", pairs))
            return got
        got = lax.all_to_all(
            blocks[0].reshape(half_devices, capacity, -1), "r", 0, 0, tiled=True
        )
        return [got.reshape(half_devices * capacity, -1)]

    def crossed(rows):
        return lax.ppermute(rows, "h", [(0, 1), (1, 0)])

    pieces = half_devices if half_devices <= FEW else 1
    other_parts = [crossed(rows) for rows in normed]
    own_in = inside(placed(own_place, normed, pieces))
    other_in = [inside(placed(other_place, [rows], pieces)) for rows in other_parts]
    places, tops = [], [0, half_devices * capacity]
    for top, parts in zip(tops, ([own_in], other_in)):
        left = 0
        for part in parts:
            places += [(top + i * part[0].shape[0], left) for i in range(len(part))]
            left += part[0].shape[1]
    x_pieces = [block for part in [own_in] + other_in for block in part]
    rows = 2 * half_devices * capacity
    near_own, near_other, x = hidden_rows(x_pieces, places, rows, gates[:far], ups[:far])
    far_own, far_other = hidden_rows([x], [], rows, gates[far:], ups[far:])
    own_hidden, other_hidden = [near_own, far_own], [near_other, far_other]

    outputs = []
    for k in (0, 1):
        across = inside(down_rows(other_hidden, downs[k], pieces))
        back = crossed(weighted(other_gates, across))
        within = inside(down_rows(own_hidden, downs[k], pieces))
        result = weighted(own_gates, within, (middle[k], back))
        rows = natural(
            exchanged(lambda bit: lax.dynamic_slice_in_dim(result, (tp ^ bit) * narrow, narrow, 1)),
            tp,
        )
        outputs.append(jnp.concatenate(rows, axis=0))
    return jnp.concatenate(outputs, axis=1)


def solution(mesh):
    count = mesh.shape["sp"]
    split = Mesh(mesh.devices.reshape(2, count // 2, -1), ("h", "r", "tp"))
    sp = ("h", "r")
    return jax.shard_map(
        shards,
        mesh=split,
        in_specs=(
            P(sp, "tp"),
            P(sp, "tp"),
            P(None, "tp"),
            P("tp"),
            P("tp"),
            P("tp", None),
            P(sp, "tp"),
            P("tp"),
            P(sp, None),
            P(sp),
            P(sp),
            P(sp, None, "tp"),
            P(sp, None, "tp"),
            P(sp, "tp", None),
        ),
        out_specs=P(sp, "tp"),
        check_vma=False,
    )
```
